32 devices in a mesh: fs: 8 (over z, x), tp: 4 (over y, core).
Axes of the slice: x: 2, y: 2, z: 4, core: 2. Of those that a mesh axis runs over, the one named last changes fastest.
Arguments:
- tokens: bfloat16 [2048, 2048], P('fs'), may hold values from -6 to 6
- norm_gain: float32 [2048], P('fs'), may hold values from 0.1 to 1.9
- gate_weight: float32 [8, 2048, 2048], P(None, 'fs', 'tp'), as said below
- up_weight: float32 [8, 2048, 2048], P(None, 'fs', 'tp'), as said below
- down_weight: float32 [8, 2048, 2048], P(None, 'fs', 'tp'), may hold values from -0.125 to 0.125
- routes: int32 [2048, 4], P('fs'), may hold values from 0 to 7, all different within a row; in each aligned block of 256 rows (0 to 255, 256 to 511, ...) at most 192 rows name the same one
- route_weights: bfloat16 [2048, 4], P('fs'), may hold values from 0.049804688 to 0.59765625
Outputs:
- gate_ready: bfloat16 [8, 2048, 2048], P('fs', None, 'tp')
- up_ready: bfloat16 [8, 2048, 2048], P('fs', None, 'tp')
- down_ready: bfloat16 [8, 2048, 2048], P('fs', None, 'tp')
- moe_output: bfloat16 [2048, 2048], P('fs', 'tp')
The draws below stay inside these ranges and needn't reach their ends.
Inputs may be any that keep to these rules, and one draw needn't show every extreme that they name: `routes`: each row names 4 different experts; among the rows of one index of fs no expert is named more than 192 times. `gate_weight`: real-valued entries, drawn afresh for each expert; the scale may differ from column to column. `up_weight`: real-valued entries, drawn afresh for each expert; the scale may differ from column to column.
All inputs are finite; a program needn't handle non-finite values.
Results may differ from the reference program's by a relative error of at most 0.015.
Values may be sent and summed in bfloat16 or wider, within the bound.
A program may use at most 128 MiB of HBM per device.

```python
import math
import jax
import jax.numpy as jnp
import numpy as np
from jax import lax

D = 2048
FF = 2048
TOP_K = 4
TOK_DEV = 256
EXPERTS = 8
CAP = 192
TOKENS = 2048
N_FS = 8
N_TP = 4


def clamped_weight(key, salt_value):
    inner_key = jax.random.fold_in(key, salt_value)
    drawn = jnp.clip(jax.random.normal(jax.random.fold_in(inner_key, 1), (EXPERTS, D, FF), jnp.float32), -6.0, 6.0) * D ** (-0.5)
    return drawn


def draw_gate_weight(key, part):
    return clamped_weight(key, 11)


def draw_up_weight(key, part):
    return clamped_weight(key, 23)


def block_levels(rng, extent, cuts, least, high):
    level = 1.0
    for axis_at, blocks in cuts:
        steps = jax.random.uniform(jax.random.fold_in(jax.random.fold_in(rng, 6), axis_at), (blocks,), jnp.float32, least / len(cuts), high / len(cuts))
        level = level * jnp.repeat(jnp.exp(steps), extent[axis_at] // blocks).reshape((-1,) + (1,) * (len(extent) - 1 - axis_at))
    return level


def shared_out(rng, own, number, rows, count, top, reach, lean):
    ranking = jax.random.permutation(rng, count)
    crowded, common = load_shares(count, rows * top, reach, lean, True), load_shares(count, rows * top, reach, lean, False)
    places = jnp.arange(count)

    def named(tallies, turn):
        used = int((tallies > 0).sum())
        fixed = max(1, used // 4)
        moved = fixed + (places - fixed + turn * (used - fixed)) % max(1, count - fixed)
        return jnp.zeros((count,), jnp.int32).at[ranking[jnp.where(places < fixed, places, moved)]].set(jnp.asarray(tallies, jnp.int32))

    tallies = jnp.where(number % 4 == 0, named(crowded, number // 4), named(common, number - number // 4 - 1))
    mixed = jax.random.permutation(jax.random.fold_in(own, 3), count)
    donor, receiver = mixed[0:count // 2 * 2:2], mixed[1:count // 2 * 2:2]
    slack = jnp.minimum(tallies[donor] - 1, reach - tallies[receiver]) // 2
    slack = jnp.where((donor == ranking[0]) | (receiver == ranking[0]) | (tallies[receiver] == 0), 0, jnp.maximum(slack, 0))
    moved = jax.random.randint(jax.random.fold_in(own, 4), (count // 2,), 0, 1 << 20) % (slack + 1)
    tallies = tallies.at[donor].add(-moved).at[receiver].add(moved)
    labels = jnp.searchsorted(jnp.cumsum(tallies), jnp.arange(rows * top), side="right").astype(jnp.int32)
    grid = labels.reshape(top, rows).T
    grid = grid[jax.random.permutation(jax.random.fold_in(own, 1), rows)]
    turn = jax.random.randint(jax.random.fold_in(own, 2), (rows, 1), 0, top)
    return jnp.take_along_axis(grid, (jnp.arange(top)[None, :] + turn) % top, axis=1)


def load_shares(amount, total, reach, skew, full):
    loads = [(1 << 20) // math.isqrt(rank ** skew) + 1 for rank in range(1, amount + 1)]
    largest = reach if full else min(reach, max(-(-total // amount), total * loads[0] // sum(loads)))
    least = 1 if total - largest >= amount - 1 else 0
    counts, rest = [largest] + [least] * (amount - 1), total - largest - least * (amount - 1)
    while rest > 0:
        movable = [i for i in range(1, amount) if counts[i] < largest] or [i for i in range(1, amount) if counts[i] < reach]
        mass, remaining = sum([loads[i] for i in movable]), rest
        for i in movable:
            extra = min(reach - counts[i], max(1, remaining * loads[i] // mass), rest)
            counts[i] = counts[i] + extra
            rest = rest - extra
    return np.array(counts)


def normal_values(own_key, shape, scale, bound, cuts=(), kind=jnp.bfloat16):
    result = scale * jax.random.normal(own_key, shape, jnp.float32)
    if cuts:
        result = result * block_levels(own_key, shape, cuts, -0.22, 0.18)
    return jnp.clip(result, -bound, bound).astype(kind)


def setup_inputs(seed: int = 0) -> dict:
    splits = jax.random.split(jax.random.key(seed), 8)
    tokens = normal_values(splits[0], (TOKENS, D), 1.0, 6.0, ((0, 8),))
    norm_gain = jnp.clip(1.0 + 0.18 * jax.random.normal(splits[1], (D,), jnp.float32), 0.1, 1.9)
    gate_weight = draw_gate_weight(jax.random.fold_in(splits[7], 71), 0)
    up_weight = draw_up_weight(jax.random.fold_in(splits[7], 71), 0)
    down_weight = normal_values(splits[4], (EXPERTS, D, FF), FF ** -0.5, 0.125, ((1, 8), (2, 4)), jnp.float32)
    routes_keys = jax.random.split(jax.random.fold_in(splits[5], 1), TOKENS // TOK_DEV)
    routes_turns = jax.random.permutation(jax.random.fold_in(splits[5], 3), TOKENS // TOK_DEV)
    routes = jax.vmap(lambda own, number: shared_out(jax.random.fold_in(splits[5], 2), own, number, TOK_DEV, EXPERTS, TOP_K, CAP, 2))(routes_keys, routes_turns).reshape((TOKENS, TOP_K))
    route_weights = jnp.clip(0.049804688 + 0.54785156 * jax.random.uniform(splits[6], (TOKENS, TOP_K), jnp.float32) ** block_levels(splits[6], (TOKENS, TOP_K), ((0, 8),), -0.2, 0.2), 0.049804688, 0.59765625).astype(jnp.bfloat16)
    return dict(tokens=tokens, norm_gain=norm_gain, gate_weight=gate_weight, up_weight=up_weight, down_weight=down_weight, routes=routes, route_weights=route_weights)


norm_eps = 1e-06
clamp_limit = 7.0
gate_alpha = 1.702

def slot_numbers(route_block, capacity, experts):
    flat_routes = route_block.reshape(-1)
    onehot = (flat_routes[:, None] == jnp.arange(experts, dtype=jnp.int32)[None, :]).astype(jnp.int32)
    earlier = jnp.cumsum(onehot, axis=0) - onehot
    position = lax.optimization_barrier(jnp.sum(earlier * onehot, axis=1))
    return (flat_routes * capacity + position).astype(jnp.int32)

def slot_sources(slots, top_count, tok_rows, total_slots):
    owners = (jnp.arange(slots.shape[0], dtype=jnp.int32) // top_count).astype(jnp.int32)
    return jnp.full((total_slots,), tok_rows, jnp.int32).at[slots].set(owners)

def combine_table(slots, weights_block, total_slots):
    matches = slots.reshape(weights_block.shape)[:, :, None] == jnp.arange(total_slots, dtype=jnp.int32)[None, None, :]
    table = lax.optimization_barrier(jnp.sum(jnp.where(matches, weights_block.astype(jnp.float32)[:, :, None], jnp.float32(0.0)), axis=1))
    return table.astype(jnp.bfloat16)

def activate(gate_pre, up_pre):
    gate_part = jnp.minimum(gate_pre, clamp_limit)
    up_part = jnp.clip(up_pre, -clamp_limit, clamp_limit)
    return (up_part + 1.0) * gate_part * jax.nn.sigmoid(gate_alpha * gate_part)

def reference(tokens, norm_gain, gate_weight, up_weight, down_weight, routes, route_weights):
    gain_col = norm_gain.astype(jnp.float32)[None, :, None]
    gate_ready = (gain_col * gate_weight).astype(jnp.bfloat16)
    up_ready = (gain_col * up_weight).astype(jnp.bfloat16)
    down_ready = down_weight.astype(jnp.bfloat16)
    wide_tokens = tokens.astype(jnp.float32)
    normed = (wide_tokens * lax.rsqrt(lax.optimization_barrier(jnp.mean(wide_tokens * wide_tokens, axis=1, keepdims=True)) + norm_eps)).astype(jnp.bfloat16)
    total_slots = EXPERTS * CAP
    route_blocks = routes.reshape(N_FS, TOK_DEV, TOP_K)
    slots = jax.vmap(lambda blk: slot_numbers(blk, CAP, EXPERTS))(route_blocks)
    sources = jax.vmap(lambda sl: slot_sources(sl, TOP_K, TOK_DEV, total_slots))(slots)
    padded = jnp.concatenate([normed.reshape(N_FS, TOK_DEV, D), jnp.zeros((N_FS, 1, D), jnp.bfloat16)], axis=1)
    dispatched = jax.vmap(lambda rows_blk, src: rows_blk[src])(padded, sources)
    per_expert = dispatched.reshape(N_FS, EXPERTS, CAP, D).transpose(1, 0, 2, 3).reshape(EXPERTS, N_FS * CAP, D)
    share = FF // N_TP

    def run_expert(operands):
        rows_in, gate_mat, up_mat, down_mat = operands
        gate_pre = jnp.dot(rows_in, gate_mat, preferred_element_type=jnp.float32)
        up_pre = jnp.dot(rows_in, up_mat, preferred_element_type=jnp.float32)
        hidden = activate(gate_pre, up_pre).astype(jnp.bfloat16)
        total = jnp.zeros((rows_in.shape[0], D), jnp.float32)
        for block_index in range(N_TP):
            hid_block = hidden[:, block_index * share:(block_index + 1) * share]
            down_block = down_mat[:, block_index * share:(block_index + 1) * share]
            partial_sum = lax.dot_general(hid_block, down_block, (((1,), (1,)), ((), ())), preferred_element_type=jnp.float32).astype(jnp.bfloat16)
            total = total + lax.optimization_barrier(partial_sum).astype(jnp.float32)
        return total.astype(jnp.bfloat16)
    expert_out = lax.map(run_expert, (per_expert, gate_ready, up_ready, down_ready))
    by_block = expert_out.reshape(EXPERTS, N_FS, CAP, D).transpose(1, 0, 2, 3).reshape(N_FS, total_slots, D)
    tables = jax.vmap(lambda sl, wb: combine_table(sl, wb, total_slots))(slots, route_weights.reshape(N_FS, TOK_DEV, TOP_K))
    mixed_rows = jnp.einsum('btj,bjd->btd', tables.astype(jnp.float32), by_block.astype(jnp.float32))
    moe_output = mixed_rows.reshape(N_FS * TOK_DEV, D).astype(jnp.bfloat16)
    return (gate_ready, up_ready, down_ready, moe_output)
```

```python
import functools

import jax
import jax.numpy as jnp
from jax import lax
from jax.experimental import pallas as pl
from jax.experimental.pallas import tpu as pltpu
from jax.sharding import PartitionSpec as P

norm_eps = 1e-06
clamp_limit = 7.0
gate_alpha = 1.702
MESH = pl.DeviceIdType.MESH
CORES = 2


def activate(gate_pre, up_pre):
    gate_part = jnp.minimum(gate_pre, clamp_limit)
    up_part = jnp.clip(up_pre, -clamp_limit, clamp_limit)
    return (up_part + 1.0) * gate_part * jax.nn.sigmoid(gate_alpha * gate_part)


def earlier_counts(member):
    rows = member.shape[1]
    before = (
        jnp.arange(rows, dtype=jnp.int32)[:, None] < jnp.arange(rows, dtype=jnp.int32)[None, :]
    ).astype(jnp.bfloat16)
    return jnp.dot(
        member.astype(jnp.bfloat16), before, preferred_element_type=jnp.float32
    ).astype(jnp.int32)


def kernel(
    n,
    groups,
    row_tile,
    sent,
    gate_local,
    up_local,
    down_local,
    gate_ready,
    up_ready,
    down_ready,
    returned,
    routed,
    hidden,
    kept,
    given,
    partner_sums,
    chip_sums,
    finished,
    dispatch_send,
    dispatch_recv,
    share_send,
    share_recv,
    weight_send,
    weight_recv,
    pair_send,
    pair_recv,
    chip_send,
    chip_recv,
    return_send,
    return_recv,
    own_sem,
):
    me = lax.axis_index("fs")
    tp = lax.axis_index("tp")
    chips = groups // CORES
    chip = tp // CORES
    core = lax.rem(tp, CORES)
    partner = chip * CORES + (CORES - 1 - core)
    capacity = sent.shape[0] // n
    source_rows = gate_local.shape[1]
    part = sent.shape[1]
    shares = n // groups
    total_slots = n * capacity

    def slots_of(block):
        return pl.ds(pl.multiple_of(block * capacity, 16), capacity)

    def rows_of(block):
        return pl.ds(pl.multiple_of(block * source_rows, 16), source_rows)

    barrier = pltpu.get_barrier_semaphore()
    for k in range(1, n):
        pl.semaphore_signal(
            barrier, inc=1, device_id=(lax.rem(me + k, n), tp), device_id_type=MESH
        )
    for k in range(1, groups):
        pl.semaphore_signal(
            barrier, inc=1, device_id=(me, lax.rem(tp + k, groups)), device_id_type=MESH
        )
    pl.semaphore_wait(barrier, n + groups - 2)

    waits = []

    dispatch = {}
    for k in range(1, n):
        peer = lax.rem(me + k, n)
        copy = pltpu.make_async_remote_copy(
            src_ref=sent.at[slots_of(peer)],
            dst_ref=routed.at[tp, slots_of(me)],
            send_sem=dispatch_send.at[k],
            recv_sem=dispatch_recv.at[k],
            device_id=(peer, tp),
            device_id_type=MESH,
        )
        copy.start()
        dispatch[k] = copy
    own_tokens = pltpu.make_async_copy(
        sent.at[slots_of(me)], routed.at[tp, slots_of(me)], own_sem.at[3]
    )
    own_tokens.start()
    own_weights = []
    weights = {}
    locals_ = (gate_local, up_local, down_local)
    readies = (gate_ready, up_ready, down_ready)
    for j in range(3):
        copy = pltpu.make_async_copy(locals_[j].at[me], readies[j].at[rows_of(me)], own_sem.at[j])
        copy.start()
        own_weights.append(copy)
    for turn in ((0, 1), (2,)):
        for k in range(1, n):
            peer = lax.rem(me + k, n)
            for j in turn:
                copy = pltpu.make_async_remote_copy(
                    src_ref=locals_[j].at[peer],
                    dst_ref=readies[j].at[rows_of(me)],
                    send_sem=weight_send.at[j, k],
                    recv_sem=weight_recv.at[j, k],
                    device_id=(peer, tp),
                    device_id_type=MESH,
                )
                copy.start()
                weights[j, k] = copy

    for k in range(n):
        source = lax.rem(me - k + n, n)
        if k == 0:
            own_tokens.wait()
        else:
            dispatch[k].wait_recv()
        for step in range(1, groups):
            pltpu.make_async_remote_copy(
                src_ref=routed.at[tp, slots_of(source)],
                dst_ref=routed.at[tp, slots_of(source)],
                send_sem=share_send.at[step],
                recv_sem=share_recv.at[step],
                device_id=(me, lax.rem(tp + step, groups)),
                device_id_type=MESH,
            ).start()
    share_waits = []
    for step in range(1, groups):
        origin = lax.rem(tp - step + groups, groups)
        share = pltpu.make_async_remote_copy(
            src_ref=routed.at[tp],
            dst_ref=routed.at[origin],
            send_sem=share_send.at[step],
            recv_sem=share_recv.at[step],
            device_id=(me, lax.rem(tp + step, groups)),
            device_id_type=MESH,
        )
        share.wait_recv()
        share_waits.append(share)

    for j in range(2):
        own_weights[j].wait()
        for k in range(1, n):
            weights[j, k].wait_recv()

    @pl.loop(0, total_slots // row_tile)
    def _(tile):
        rows = pl.ds(pl.multiple_of(tile * row_tile, 16), row_tile)
        gate_pre = jnp.zeros((row_tile, hidden.shape[1]), jnp.float32)
        up_pre = jnp.zeros((row_tile, hidden.shape[1]), jnp.float32)
        for t in range(groups):
            piece = routed[t, rows, :]
            gate_pre += jnp.dot(
                piece, gate_ready[t * part : (t + 1) * part], preferred_element_type=jnp.float32
            )
            up_pre += jnp.dot(
                piece, up_ready[t * part : (t + 1) * part], preferred_element_type=jnp.float32
            )
        hidden[rows, :] = activate(gate_pre, up_pre).astype(jnp.bfloat16)

    own_weights[2].wait()

    def arrival(source):
        k = lax.rem(me - source + n, n)

        @pl.when(k > 0)
        def _():
            pltpu.make_async_remote_copy(
                src_ref=down_local.at[0],
                dst_ref=down_ready.at[rows_of(source)],
                send_sem=weight_send.at[2, k],
                recv_sem=weight_recv.at[2, k],
                device_id=(me, partner),
                device_id_type=MESH,
            ).wait_recv()

    def project(source, out, slot):
        down = down_ready[rows_of(source), :]

        @pl.loop(0, total_slots // row_tile)
        def _(tile):
            rows = pl.ds(pl.multiple_of(tile * row_tile, 16), row_tile)
            out[slot, rows, :] = lax.dot_general(
                hidden[rows, :], down, (((1,), (1,)), ((), ())), preferred_element_type=jnp.float32
            ).astype(jnp.bfloat16)

    sums = []
    order = [(h, r) for h in range(1, chips) for r in range(shares)]
    order += [(0, r) for r in range(shares)]

    def start_group(h, r):
        slot = h * shares + r
        to_chip = lax.rem(chip + h, chips)
        give_source = (to_chip * CORES + (CORES - 1 - core)) * shares + r
        keep_source = (to_chip * CORES + core) * shares + r
        arrival(give_source)
        project(give_source, given, slot)
        pair = pltpu.make_async_remote_copy(
            src_ref=given.at[slot],
            dst_ref=partner_sums.at[slot],
            send_sem=pair_send.at[slot],
            recv_sem=pair_recv.at[slot],
            device_id=(me, partner),
            device_id_type=MESH,
        )
        pair.start()
        arrival(keep_source)
        project(keep_source, kept, slot)
        return pair

    for h, r in order:
        slot = h * shares + r
        pair = start_group(h, r)
        pair.wait_recv()
        waits.append(pair)
        if h > 0:

            @pl.loop(0, total_slots // row_tile)
            def _(tile):
                rows = pl.ds(pl.multiple_of(tile * row_tile, 16), row_tile)
                total = kept[slot, rows, :].astype(jnp.float32)
                total += partner_sums[slot, rows, :].astype(jnp.float32)
                kept[slot, rows, :] = total.astype(jnp.bfloat16)

            over = pltpu.make_async_remote_copy(
                src_ref=kept.at[slot],
                dst_ref=chip_sums.at[slot - shares],
                send_sem=chip_send.at[slot - shares],
                recv_sem=chip_recv.at[slot - shares],
                device_id=(me, lax.rem(chip + h, chips) * CORES + core),
                device_id_type=MESH,
            )
            over.start()
            sums.append((r, over))
            waits.append(over)
        else:
            for share, over in sums:
                if share == r:
                    over.wait_recv()

            @pl.loop(0, total_slots // row_tile)
            def _(tile):
                rows = pl.ds(pl.multiple_of(tile * row_tile, 16), row_tile)
                total = kept[slot, rows, :].astype(jnp.float32)
                total += partner_sums[slot, rows, :].astype(jnp.float32)
                for other in range(1, chips):
                    total += chip_sums[(other - 1) * shares + r, rows, :].astype(jnp.float32)
                finished[r, rows, :] = total.astype(jnp.bfloat16)

            for k in range(1, n):
                peer = lax.rem(me + k, n)
                back = pltpu.make_async_remote_copy(
                    src_ref=finished.at[r, slots_of(peer)],
                    dst_ref=returned.at[r, slots_of(me)],
                    send_sem=return_send.at[r, k],
                    recv_sem=return_recv.at[r, k],
                    device_id=(peer, tp),
                    device_id_type=MESH,
                )
                back.start()
                waits.append(back)
                sums.append((-1, back))
            own = pltpu.make_async_copy(
                finished.at[r, slots_of(me)], returned.at[r, slots_of(me)], own_sem.at[4 + r]
            )
            own.start()
            own_weights.append(own)

    for share, back in sums:
        if share == -1:
            back.wait_recv()
    for own in own_weights[3:]:
        own.wait()
    for copy in waits + share_waits + list(dispatch.values()) + list(weights.values()):
        copy.wait_send()


def hand_over(sent, gate_local, up_local, down_local):
    n = lax.axis_size("fs")
    groups = lax.axis_size("tp")
    total_slots, part = sent.shape
    source_rows, units = gate_local.shape[1:]
    width = n * source_rows
    shares = n // groups
    chips = groups // CORES
    vmem = pl.BlockSpec(memory_space=pltpu.VMEM)
    anywhere = pl.BlockSpec(memory_space=pl.ANY)
    bf16 = jnp.bfloat16
    ready = jax.ShapeDtypeStruct((width, units), bf16)
    dma = pltpu.SemaphoreType.DMA
    return pl.pallas_call(
        functools.partial(kernel, n, groups, total_slots // 4),
        out_shape=(
            ready,
            ready,
            ready,
            jax.ShapeDtypeStruct((shares, total_slots, source_rows), bf16),
        ),
        in_specs=[anywhere] * 4,
        out_specs=(vmem,) * 4,
        scratch_shapes=[
            pltpu.VMEM((groups, total_slots, part), bf16),
            pltpu.VMEM((total_slots, units), bf16),
            pltpu.VMEM((chips * shares, total_slots, source_rows), bf16),
            pltpu.VMEM((chips * shares, total_slots, source_rows), bf16),
            pltpu.VMEM((chips * shares, total_slots, source_rows), bf16),
            pltpu.VMEM(((chips - 1) * shares, total_slots, source_rows), bf16),
            pltpu.VMEM((shares, total_slots, source_rows), bf16),
            dma((n,)),
            dma((n,)),
            dma((groups,)),
            dma((groups,)),
            dma((3, n)),
            dma((3, n)),
            dma((chips * shares,)),
            dma((chips * shares,)),
            dma(((chips - 1) * shares,)),
            dma(((chips - 1) * shares,)),
            dma((shares, n)),
            dma((shares, n)),
            dma((4 + shares,)),
        ],
        compiler_params=pltpu.CompilerParams(
            collective_id=0, has_side_effects=True, vmem_limit_bytes=52 * 1024 * 1024
        ),
    )(sent, gate_local, up_local, down_local)


def body(tokens, norm_gain, gate_weight, up_weight, down_weight, routes, route_weights):
    experts = lax.axis_size("fs")
    groups = lax.axis_size("tp")
    tok_rows, model_width = tokens.shape
    top_count = routes.shape[1]
    capacity = 3 * tok_rows * top_count // (2 * experts)
    total_slots = experts * capacity
    part_width = model_width // groups

    gate_local = (norm_gain[None, :, None] * gate_weight).astype(jnp.bfloat16)
    up_local = (norm_gain[None, :, None] * up_weight).astype(jnp.bfloat16)
    down_local = down_weight.astype(jnp.bfloat16)

    wide_tokens = tokens.astype(jnp.float32)
    scale = lax.rsqrt(jnp.mean(wide_tokens * wide_tokens, axis=1, keepdims=True) + norm_eps)
    start = lax.axis_index("tp") * part_width
    columns = (
        lax.dynamic_slice_in_dim(tokens, start, part_width, 1).astype(jnp.float32) * scale
    ).astype(jnp.bfloat16)

    chosen = routes.T[:, None, :] == jnp.arange(experts, dtype=jnp.int32)[None, :, None]
    member = jnp.sum(chosen.astype(jnp.int32), axis=0)
    position = jnp.where(member > 0, earlier_counts(member), -1)
    row_weight = jnp.sum(
        jnp.where(chosen, route_weights.T.astype(jnp.float32)[:, None, :], 0.0), axis=0
    )
    here = position[:, None, :] == jnp.arange(capacity, dtype=jnp.int32)[None, :, None]
    pick = here.astype(jnp.bfloat16).reshape(total_slots, tok_rows)
    table = (
        jnp.where(here, row_weight[:, None, :], jnp.float32(0.0))
        .astype(jnp.bfloat16)
        .reshape(total_slots, tok_rows)
    )
    sent = jnp.dot(pick, columns, preferred_element_type=jnp.float32).astype(jnp.bfloat16)

    gate_ready, up_ready, down_ready, returned = hand_over(
        sent, gate_local, up_local, down_local
    )
    moe_output = jnp.concatenate(
        [
            lax.dot_general(
                table, piece, (((0,), (0,)), ((), ())), preferred_element_type=jnp.float32
            ).astype(jnp.bfloat16)
            for piece in returned
        ],
        axis=1,
    )
    return (gate_ready[None], up_ready[None], down_ready[None], moe_output)


def solution(mesh):
    in_specs = (
        P("fs", None),
        P("fs"),
        P(None, "fs", "tp"),
        P(None, "fs", "tp"),
        P(None, "fs", "tp"),
        P("fs", None),
        P("fs", None),
    )
    out_specs = (P("fs", None, "tp"), P("fs", None, "tp"), P("fs", None, "tp"), P("fs", "tp"))
    return jax.shard_map(body, mesh=mesh, in_specs=in_specs, out_specs=out_specs, check_vma=False)
```

```python
import functools

import jax
import jax.numpy as jnp
from jax import lax
from jax.experimental import pallas as pl
from jax.experimental.pallas import tpu as pltpu
from jax.sharding import PartitionSpec as P

norm_eps = 1e-06
clamp_limit = 7.0
gate_alpha = 1.702
MESH = pl.DeviceIdType.MESH
CORES = 2
DEPTH = 4


def activate(gate_pre, up_pre):
    gate_part = jnp.minimum(gate_pre, clamp_limit)
    up_part = jnp.clip(up_pre, -clamp_limit, clamp_limit)
    return (up_part + 1.0) * gate_part * jax.nn.sigmoid(gate_alpha * gate_part)


def earlier_counts(member):
    rows = member.shape[1]
    before = (
        jnp.arange(rows, dtype=jnp.int32)[:, None] < jnp.arange(rows, dtype=jnp.int32)[None, :]
    ).astype(jnp.bfloat16)
    return jnp.dot(
        member.astype(jnp.bfloat16), before, preferred_element_type=jnp.float32
    ).astype(jnp.int32)


def kernel(
    n,
    groups,
    row_tile,
    sent,
    gain,
    gate_local,
    up_local,
    down_local,
    gate_ready,
    up_ready,
    down_ready,
    returned,
    routed,
    hidden,
    kept,
    given,
    partner_sums,
    chip_sums,
    finished,
    wide,
    staged,
    dispatch_send,
    dispatch_recv,
    share_send,
    share_recv,
    weight_send,
    weight_recv,
    pair_send,
    pair_recv,
    chip_send,
    chip_recv,
    return_send,
    return_recv,
    own_sem,
    wide_sem,
):
    me = lax.axis_index("fs")
    tp = lax.axis_index("tp")
    chips = groups // CORES
    chip = tp // CORES
    core = lax.rem(tp, CORES)
    partner = chip * CORES + (CORES - 1 - core)
    capacity = sent.shape[0] // n
    source_rows = gate_local.shape[1]
    part = sent.shape[1]
    shares = n // groups
    total_slots = n * capacity

    def slots_of(block):
        return pl.ds(pl.multiple_of(block * capacity, 16), capacity)

    def rows_of(block):
        return pl.ds(pl.multiple_of(block * source_rows, 16), source_rows)

    locals_ = (gate_local, up_local, down_local)
    readies = (gate_ready, up_ready, down_ready)
    blocks = [(j, k) for turn in ((0, 1), (2,)) for k in range(n) for j in turn]

    def fetch(i):
        j, k = blocks[i]
        copy = pltpu.make_async_copy(
            locals_[j].at[lax.rem(me + k, n)], wide.at[i % DEPTH], wide_sem.at[i % DEPTH]
        )
        copy.start()
        return copy

    fetches = [fetch(i) for i in range(DEPTH)]

    barrier = pltpu.get_barrier_semaphore()
    for k in range(1, n):
        pl.semaphore_signal(
            barrier, inc=1, device_id=(lax.rem(me + k, n), tp), device_id_type=MESH
        )
    for k in range(1, groups):
        pl.semaphore_signal(
            barrier, inc=1, device_id=(me, lax.rem(tp + k, groups)), device_id_type=MESH
        )
    pl.semaphore_wait(barrier, n + groups - 2)

    waits = []

    dispatch = {}
    for k in range(1, n):
        peer = lax.rem(me + k, n)
        copy = pltpu.make_async_remote_copy(
            src_ref=sent.at[slots_of(peer)],
            dst_ref=routed.at[tp, slots_of(me)],
            send_sem=dispatch_send.at[k],
            recv_sem=dispatch_recv.at[k],
            device_id=(peer, tp),
            device_id_type=MESH,
        )
        copy.start()
        dispatch[k] = copy
    own_tokens = pltpu.make_async_copy(
        sent.at[slots_of(me)], routed.at[tp, slots_of(me)], own_sem.at[0]
    )
    own_tokens.start()
    own_copies = []
    weights = {}

    def send(j, k):
        copy = pltpu.make_async_remote_copy(
            src_ref=staged.at[j, k - 1],
            dst_ref=readies[j].at[rows_of(me)],
            send_sem=weight_send.at[j, k],
            recv_sem=weight_recv.at[j, k],
            device_id=(lax.rem(me + k, n), tp),
            device_id_type=MESH,
        )
        copy.start()
        weights[j, k] = copy

    for i, (j, k) in enumerate(blocks):
        fetches[i].wait()
        value = wide[i % DEPTH]
        if j < 2:
            value = gain[...] * value
        if k == 0:
            readies[j][rows_of(me), :] = value.astype(jnp.bfloat16)
        else:
            staged[j, k - 1] = value.astype(jnp.bfloat16)
        if i + DEPTH < len(blocks):
            fetches.append(fetch(i + DEPTH))
        if i > 0 and blocks[i - 1][1] > 0:
            send(*blocks[i - 1])
    send(*blocks[-1])

    for k in range(n):
        source = lax.rem(me - k + n, n)
        if k == 0:
            own_tokens.wait()
        else:
            dispatch[k].wait_recv()
        for step in range(1, groups):
            pltpu.make_async_remote_copy(
                src_ref=routed.at[tp, slots_of(source)],
                dst_ref=routed.at[tp, slots_of(source)],
                send_sem=share_send.at[step],
                recv_sem=share_recv.at[step],
                device_id=(me, lax.rem(tp + step, groups)),
                device_id_type=MESH,
            ).start()
    share_waits = []
    for step in range(1, groups):
        origin = lax.rem(tp - step + groups, groups)
        share = pltpu.make_async_remote_copy(
            src_ref=routed.at[tp],
            dst_ref=routed.at[origin],
            send_sem=share_send.at[step],
            recv_sem=share_recv.at[step],
            device_id=(me, lax.rem(tp + step, groups)),
            device_id_type=MESH,
        )
        share.wait_recv()
        share_waits.append(share)

    for j in range(2):
        for k in range(1, n):
            weights[j, k].wait_recv()

    @pl.loop(0, total_slots // row_tile)
    def _(tile):
        rows = pl.ds(pl.multiple_of(tile * row_tile, 16), row_tile)
        gate_pre = jnp.zeros((row_tile, hidden.shape[1]), jnp.float32)
        up_pre = jnp.zeros((row_tile, hidden.shape[1]), jnp.float32)
        for t in range(groups):
            piece = routed[t, rows, :]
            gate_pre += jnp.dot(
                piece, gate_ready[t * part : (t + 1) * part], preferred_element_type=jnp.float32
            )
            up_pre += jnp.dot(
                piece, up_ready[t * part : (t + 1) * part], preferred_element_type=jnp.float32
            )
        hidden[rows, :] = activate(gate_pre, up_pre).astype(jnp.bfloat16)

    def arrival(source):
        k = lax.rem(me - source + n, n)

        @pl.when(k > 0)
        def _():
            pltpu.make_async_remote_copy(
                src_ref=staged.at[2, 0],
                dst_ref=down_ready.at[rows_of(source)],
                send_sem=weight_send.at[2, k],
                recv_sem=weight_recv.at[2, k],
                device_id=(me, partner),
                device_id_type=MESH,
            ).wait_recv()

    def project(source, out, slot):
        down = down_ready[rows_of(source), :]

        @pl.loop(0, total_slots // row_tile)
        def _(tile):
            rows = pl.ds(pl.multiple_of(tile * row_tile, 16), row_tile)
            out[slot, rows, :] = lax.dot_general(
                hidden[rows, :], down, (((1,), (1,)), ((), ())), preferred_element_type=jnp.float32
            ).astype(jnp.bfloat16)

    sums = []
    order = [(h, r) for h in range(1, chips) for r in range(shares)]
    order += [(0, r) for r in range(shares)]

    def start_group(h, r):
        slot = h * shares + r
        to_chip = lax.rem(chip + h, chips)
        give_source = (to_chip * CORES + (CORES - 1 - core)) * shares + r
        keep_source = (to_chip * CORES + core) * shares + r
        arrival(give_source)
        project(give_source, given, slot)
        pair = pltpu.make_async_remote_copy(
            src_ref=given.at[slot],
            dst_ref=partner_sums.at[slot],
            send_sem=pair_send.at[slot],
            recv_sem=pair_recv.at[slot],
            device_id=(me, partner),
            device_id_type=MESH,
        )
        pair.start()
        arrival(keep_source)
        project(keep_source, kept, slot)
        return pair

    for h, r in order:
        slot = h * shares + r
        pair = start_group(h, r)
        pair.wait_recv()
        waits.append(pair)
        if h > 0:

            @pl.loop(0, total_slots // row_tile)
            def _(tile):
                rows = pl.ds(pl.multiple_of(tile * row_tile, 16), row_tile)
                total = kept[slot, rows, :].astype(jnp.float32)
                total += partner_sums[slot, rows, :].astype(jnp.float32)
                kept[slot, rows, :] = total.astype(jnp.bfloat16)

            over = pltpu.make_async_remote_copy(
                src_ref=kept.at[slot],
                dst_ref=chip_sums.at[slot - shares],
                send_sem=chip_send.at[slot - shares],
                recv_sem=chip_recv.at[slot - shares],
                device_id=(me, lax.rem(chip + h, chips) * CORES + core),
                device_id_type=MESH,
            )
            over.start()
            sums.append((r, over))
            waits.append(over)
        else:
            for share, over in sums:
                if share == r:
                    over.wait_recv()

            @pl.loop(0, total_slots // row_tile)
            def _(tile):
                rows = pl.ds(pl.multiple_of(tile * row_tile, 16), row_tile)
                total = kept[slot, rows, :].astype(jnp.float32)
                total += partner_sums[slot, rows, :].astype(jnp.float32)
                for other in range(1, chips):
                    total += chip_sums[(other - 1) * shares + r, rows, :].astype(jnp.float32)
                finished[r, rows, :] = total.astype(jnp.bfloat16)

            for k in range(1, n):
                peer = lax.rem(me + k, n)
                back = pltpu.make_async_remote_copy(
                    src_ref=finished.at[r, slots_of(peer)],
                    dst_ref=returned.at[r, slots_of(me)],
                    send_sem=return_send.at[r, k],
                    recv_sem=return_recv.at[r, k],
                    device_id=(peer, tp),
                    device_id_type=MESH,
                )
                back.start()
                waits.append(back)
                sums.append((-1, back))
            own = pltpu.make_async_copy(
                finished.at[r, slots_of(me)], returned.at[r, slots_of(me)], own_sem.at[1 + r]
            )
            own.start()
            own_copies.append(own)

    for share, back in sums:
        if share == -1:
            back.wait_recv()
    for own in own_copies:
        own.wait()
    for copy in waits + share_waits + list(dispatch.values()) + list(weights.values()):
        copy.wait_send()


def hand_over(sent, gain, gate_local, up_local, down_local):
    n = lax.axis_size("fs")
    groups = lax.axis_size("tp")
    total_slots, part = sent.shape
    source_rows, units = gate_local.shape[1:]
    width = n * source_rows
    shares = n // groups
    chips = groups // CORES
    vmem = pl.BlockSpec(memory_space=pltpu.VMEM)
    anywhere = pl.BlockSpec(memory_space=pl.ANY)
    bf16 = jnp.bfloat16
    ready = jax.ShapeDtypeStruct((width, units), bf16)
    dma = pltpu.SemaphoreType.DMA
    return pl.pallas_call(
        functools.partial(kernel, n, groups, total_slots // 4),
        out_shape=(
            ready,
            ready,
            ready,
            jax.ShapeDtypeStruct((shares, total_slots, source_rows), bf16),
        ),
        in_specs=[anywhere, vmem] + [anywhere] * 3,
        out_specs=(vmem,) * 4,
        scratch_shapes=[
            pltpu.VMEM((groups, total_slots, part), bf16),
            pltpu.VMEM((total_slots, units), bf16),
            pltpu.VMEM((chips * shares, total_slots, source_rows), bf16),
            pltpu.VMEM((chips * shares, total_slots, source_rows), bf16),
            pltpu.VMEM((chips * shares, total_slots, source_rows), bf16),
            pltpu.VMEM(((chips - 1) * shares, total_slots, source_rows), bf16),
            pltpu.VMEM((shares, total_slots, source_rows), bf16),
            pltpu.VMEM((DEPTH, source_rows, units), jnp.float32),
            pltpu.VMEM((3, n - 1, source_rows, units), bf16),
            dma((n,)),
            dma((n,)),
            dma((groups,)),
            dma((groups,)),
            dma((3, n)),
            dma((3, n)),
            dma((chips * shares,)),
            dma((chips * shares,)),
            dma(((chips - 1) * shares,)),
            dma(((chips - 1) * shares,)),
            dma((shares, n)),
            dma((shares, n)),
            dma((1 + shares,)),
            dma((DEPTH,)),
        ],
        compiler_params=pltpu.CompilerParams(
            collective_id=0, has_side_effects=True, vmem_limit_bytes=52 * 1024 * 1024
        ),
    )(sent, gain, gate_local, up_local, down_local)


def body(tokens, norm_gain, gate_weight, up_weight, down_weight, routes, route_weights):
    experts = lax.axis_size("fs")
    groups = lax.axis_size("tp")
    tok_rows, model_width = tokens.shape
    top_count = routes.shape[1]
    capacity = 3 * tok_rows * top_count // (2 * experts)
    total_slots = experts * capacity
    part_width = model_width // groups

    wide_tokens = tokens.astype(jnp.float32)
    scale = lax.rsqrt(jnp.mean(wide_tokens * wide_tokens, axis=1, keepdims=True) + norm_eps)
    start = lax.axis_index("tp") * part_width
    columns = (
        lax.dynamic_slice_in_dim(tokens, start, part_width, 1).astype(jnp.float32) * scale
    ).astype(jnp.bfloat16)

    chosen = routes.T[:, None, :] == jnp.arange(experts, dtype=jnp.int32)[None, :, None]
    member = jnp.sum(chosen.astype(jnp.int32), axis=0)
    position = jnp.where(member > 0, earlier_counts(member), -1)
    row_weight = jnp.sum(
        jnp.where(chosen, route_weights.T.astype(jnp.float32)[:, None, :], 0.0), axis=0
    )
    here = position[:, None, :] == jnp.arange(capacity, dtype=jnp.int32)[None, :, None]
    pick = here.astype(jnp.bfloat16).reshape(total_slots, tok_rows)
    table = (
        jnp.where(here, row_weight[:, None, :], jnp.float32(0.0))
        .astype(jnp.bfloat16)
        .reshape(total_slots, tok_rows)
    )
    sent = jnp.dot(pick, columns, preferred_element_type=jnp.float32).astype(jnp.bfloat16)

    gate_ready, up_ready, down_ready, returned = hand_over(
        sent, norm_gain[:, None], gate_weight, up_weight, down_weight
    )
    moe_output = jnp.concatenate(
        [
            lax.dot_general(
                table, piece, (((0,), (0,)), ((), ())), preferred_element_type=jnp.float32
            ).astype(jnp.bfloat16)
            for piece in returned
        ],
        axis=1,
    )
    return (gate_ready[None], up_ready[None], down_ready[None], moe_output)


def solution(mesh):
    in_specs = (
        P("fs", None),
        P("fs"),
        P(None, "fs", "tp"),
        P(None, "fs", "tp"),
        P(None, "fs", "tp"),
        P("fs", None),
        P("fs", None),
    )
    out_specs = (P("fs", None, "tp"), P("fs", None, "tp"), P("fs", None, "tp"), P("fs", "tp"))
    return jax.shard_map(body, mesh=mesh, in_specs=in_specs, out_specs=out_specs, check_vma=False)
```
